32 devices in a mesh: ep: 8 (over z, core), tp: 4 (over y, x).
Axes of the slice: x: 2, y: 2, z: 4, core: 2. Of those that a mesh axis runs over, the one named last changes fastest.
Arguments:
- mixer_input: bfloat16 [2048, 1024], P('ep', 'tp'), may hold values from -6 to 6
- log_step: float32 [64], P('tp'), may hold values from -12.8 to -2.7
- decay_shift: float32 [2048, 64], P('ep', 'tp'), may hold values from -2 to 0
- input_map: bfloat16 [2, 64, 64, 16], P(None, 'tp'), may hold values from -71.55418 to 71.55418
- readout: float32 [2, 64, 16, 64], P(None, 'tp'), may hold values from -0.5 to 0.5
- mixer_weight: bfloat16 [1024, 2048], P(None, 'tp'), may hold values from -0.1875 to 0.1875
- expert_input: bfloat16 [1024, 2048], P('ep'), may hold values from -6 to 6
- norm_gain: float32 [2048], replicated, may hold values from 0.1 to 1.9
- routes: int32 [1024, 2], P('ep'), may hold values from 0 to 7, all different within a row; in each aligned block of 128 rows (0 to 127, 128 to 255, ...) at most 64 rows name the same one
- route_weight: float32 [1024, 2], P('ep'), may hold values from 0.1 to 2.5
- expert_switch_matrix: bfloat16 [8, 2048, 4096], P('ep', None, 'tp'), may hold values from -0.125 to 0.125
- up_weight: bfloat16 [8, 2048, 4096], P('ep', None, 'tp'), may hold values from -0.125 to 0.125
- down_weight: bfloat16 [8, 4096, 2048], P('ep', None, 'tp'), may hold values from -0.09375 to 0.09375
- shared_gate: bfloat16 [2048, 1024], P(None, 'tp'), may hold values from -0.125 to 0.125
- shared_up: bfloat16 [2048, 1024], P(None, 'tp'), may hold values from -0.125 to 0.125
- shared_down: bfloat16 [1024, 2048], P(None, 'tp'), may hold values from -0.1875 to 0.1875
Outputs:
- mixer_out: bfloat16 [2048, 2048], P('ep', 'tp')
- experts_out: bfloat16 [1024, 2048], P('ep', 'tp')
The draws below stay inside these ranges and needn't reach their ends.
Inputs may be any that keep to these rules, and one draw needn't show every extreme that they name: `routes`: each row names 2 different experts. In each aligned block of 128 rows (the rows of one index of ep) no expert is named by more than 64 rows, and in some block one expert is named by exactly 64 rows.
All inputs are finite; a program needn't handle non-finite values.
Results may differ from the reference program's by a relative error of at most 0.0069.
Values may be sent and summed in bfloat16 or wider, within the bound.
No kernel may reach another device: no remote copies, remote signals or barrier semaphores. Data moves between devices by JAX's collectives and lax.ppermute only.
A program may use at most 128 MiB of HBM per device.

```python
import math
import jax
import jax.numpy as jnp
import numpy as np
from jax import lax

D = 2048
GROUPS = 64
GROUP = 16
STATE = 64
EXPERT_FF = 4096
FF = 1024
TOPK = 2
MIX_ROWS = 256
EXP_ROWS = 128
D_SSM = 1024
MIX_TOKENS = 2048
EXP_TOKENS = 1024
EXPERTS = 8
CAP = 64
N_EP = 8


def draw_steps(key):
    pick_key, fast_key, slow_key = jax.random.split(key, 3)
    quick = jax.random.randint(pick_key, (GROUPS,), 0, 2) < 1
    fast = jax.random.uniform(fast_key, (GROUPS,), jnp.float32, math.log(0.02), math.log(0.067))
    slow = jax.random.uniform(slow_key, (GROUPS,), jnp.float32, math.log(0.2), math.log(1.2)) - math.log(MIX_TOKENS)
    return jnp.where(quick, fast, slow)


def draw_log_step(key, part):
    return draw_steps(jax.random.fold_in(key, 101))


def draw_input_map(key, part):
    steps = draw_steps(jax.random.fold_in(key, 101))
    noise_key = jax.random.fold_in(key, 202)
    noise = jax.random.truncated_normal(noise_key, -4.0, 4.0, (2, GROUPS, STATE, GROUP), jnp.float32)
    scale = jnp.exp(-0.5 * steps)[None, :, None, None] / math.sqrt(2.0 * GROUP)
    return (noise * scale).astype(jnp.bfloat16)


def draw_decay_shift(key, part):
    rate_key, place_key, depth_key = jax.random.split(jax.random.fold_in(key, 303), 3)
    block_count = MIX_TOKENS // MIX_ROWS
    lowest, highest = (0.05, 0.4)
    block_rate = jnp.exp(jax.random.uniform(rate_key, (block_count, GROUPS), jnp.float32, math.log(lowest), math.log(highest))) / MIX_TOKENS
    shift_magnitude = -jnp.repeat(block_rate, MIX_ROWS, axis=0)
    capacity_indices = jax.random.randint(place_key, (2, GROUPS), 0, MIX_TOKENS)
    stack_levels = jnp.log(jax.random.uniform(depth_key, (2, GROUPS), jnp.float32, 0.55, 0.8))
    element_ordinals = jnp.arange(MIX_TOKENS, dtype=jnp.int32)[:, None, None]
    sequence_groupings = jnp.sum(jnp.where(element_ordinals == capacity_indices[None], stack_levels[None], 0.0), axis=1)
    return shift_magnitude + sequence_groupings


def steps_of(key, shape, pieces, least, high):
    def one(axis_at, blocks):
        steps = jax.random.uniform(jax.random.fold_in(jax.random.fold_in(key, 6), axis_at), (blocks,), jnp.float32, least / len(pieces), high / len(pieces))
        return jnp.repeat(jnp.exp(steps), shape[axis_at] // blocks).reshape((-1,) + (1,) * (len(shape) - axis_at - 1))

    level = one(*pieces[0])
    for cut in pieces[1:]:
        level = level * one(*cut)
    return level


def routed_block(key, own, number, rows, count, top, reach, slope):
    sequence = jax.random.permutation(key, count)
    crowded, common = load_shares(count, rows * top, reach, slope, True), load_shares(count, rows * top, reach, slope, False)
    places = jnp.arange(count)

    def named(tallies, turn):
        used = int((tallies > 0).sum())
        fixed = max(1, used // 4)
        shifted = fixed + (places - fixed + turn * (used - fixed)) % max(1, count - fixed)
        return jnp.zeros((count,), jnp.int32).at[sequence[jnp.where(places < fixed, places, shifted)]].set(jnp.asarray(tallies, jnp.int32))

    tallies = jnp.where(number % 4 == 0, named(crowded, number // 4), named(common, number - number // 4 - 1))
    mixed = jax.random.permutation(jax.random.fold_in(own, 3), count)
    donor, receiver = mixed[0:count // 2 * 2:2], mixed[1:count // 2 * 2:2]
    room = jnp.minimum(tallies[donor] - 1, reach - tallies[receiver]) // 2
    room = jnp.where((donor == sequence[0]) | (receiver == sequence[0]) | (tallies[receiver] == 0), 0, jnp.maximum(room, 0))
    shifted = jax.random.randint(jax.random.fold_in(own, 4), (count // 2,), 0, 1 << 20) % (room + 1)
    tallies = tallies.at[donor].add(-shifted).at[receiver].add(shifted)
    items = jnp.searchsorted(jnp.cumsum(tallies), jnp.arange(rows * top), side="right").astype(jnp.int32)
    table = items.reshape(top, rows).T
    table = table[jax.random.permutation(jax.random.fold_in(own, 1), rows)]
    turn = jax.random.randint(jax.random.fold_in(own, 2), (rows, 1), 0, top)
    return jnp.take_along_axis(table, (jnp.arange(top)[None, :] + turn) % top, axis=1)


def load_shares(amount, total, most, lean, full):
    weights = [(1 << 20) // math.isqrt(rank ** lean) + 1 for rank in range(1, amount + 1)]
    largest = most if full else min(most, max(-(-total // amount), total * weights[0] // sum(weights)))
    least = 1 if total - largest >= amount - 1 else 0
    holding, surplus = [largest] + [least] * (amount - 1), total - largest - least * (amount - 1)
    while surplus > 0:
        free = [i for i in range(1, amount) if holding[i] < largest] or [i for i in range(1, amount) if holding[i] < most]
        pool, remaining = sum([weights[i] for i in free]), surplus
        for i in free:
            addition = min(most - holding[i], max(1, remaining * weights[i] // pool), surplus)
            holding[i] = holding[i] + addition
            surplus = surplus - addition
    return np.array(holding)


def normal_values(key, shape, scale, bound, cuts=(), held_as=jnp.bfloat16):
    drawn = jax.random.normal(key, shape, jnp.float32) * scale
    if len(cuts) > 0:
        drawn = steps_of(key, shape, cuts, -0.22, 0.18) * drawn
    return jnp.clip(drawn, min=-bound, max=bound).astype(held_as)


def setup_inputs(seed: int = 0) -> dict:
    arg_keys = jax.random.split(jax.random.key(seed), 17)
    mixer_input = normal_values(arg_keys[0], (MIX_TOKENS, D_SSM), 1.0, 6.0, ((0, 8), (1, 4)))
    log_step = draw_log_step(jax.random.fold_in(arg_keys[16], 71), 0)
    decay_shift = draw_decay_shift(jax.random.fold_in(arg_keys[16], 71), 0)
    input_map = draw_input_map(jax.random.fold_in(arg_keys[16], 71), 0)
    readout = normal_values(arg_keys[4], (2, GROUPS, GROUP, STATE), (2 * STATE) ** -0.5, 0.5, ((1, 4),), jnp.float32)
    mixer_weight = normal_values(arg_keys[5], (D_SSM, D), D_SSM ** -0.5, 0.1875, ((1, 4),))
    expert_input = normal_values(arg_keys[6], (EXP_TOKENS, D), 1.0, 6.0, ((0, 8),))
    norm_gain = jnp.clip(1.0 + 0.18 * jax.random.normal(arg_keys[7], (D,), jnp.float32), 0.1, 1.9)
    routes_keys = jax.random.split(jax.random.fold_in(arg_keys[8], 1), EXP_TOKENS // EXP_ROWS)
    routes_turns = jax.random.permutation(jax.random.fold_in(arg_keys[8], 3), EXP_TOKENS // EXP_ROWS)
    routes = jax.vmap(lambda own, number: routed_block(jax.random.fold_in(arg_keys[8], 2), own, number, EXP_ROWS, EXPERTS, TOPK, CAP, 1))(routes_keys, routes_turns).reshape((EXP_TOKENS, TOPK))
    route_weight = jnp.clip(jnp.exp(math.log(2.5) - 3.218876 * jax.random.uniform(arg_keys[9], (EXP_TOKENS, TOPK), jnp.float32) ** steps_of(arg_keys[9], (EXP_TOKENS, TOPK), ((0, 8),), -0.2, 0.2)), 0.1, 2.5)
    expert_switch_matrix = normal_values(arg_keys[10], (EXPERTS, D, EXPERT_FF), D ** -0.5, 0.125, ((0, 8), (2, 4)))
    up_weight = normal_values(arg_keys[11], (EXPERTS, D, EXPERT_FF), D ** -0.5, 0.125, ((0, 8), (2, 4)))
    down_weight = normal_values(arg_keys[12], (EXPERTS, EXPERT_FF, D), EXPERT_FF ** -0.5, 0.09375, ((0, 8), (2, 4)))
    shared_gate = normal_values(arg_keys[13], (D, FF), D ** -0.5, 0.125, ((1, 4),))
    shared_up = normal_values(arg_keys[14], (D, FF), D ** -0.5, 0.125, ((1, 4),))
    shared_down = normal_values(arg_keys[15], (FF, D), FF ** -0.5, 0.1875, ((1, 4),))
    return {"mixer_input": mixer_input, "log_step": log_step, "decay_shift": decay_shift, "input_map": input_map, "readout": readout, "mixer_weight": mixer_weight, "expert_input": expert_input, "norm_gain": norm_gain, "routes": routes, "route_weight": route_weight, "expert_switch_matrix": expert_switch_matrix, "up_weight": up_weight, "down_weight": down_weight, "shared_gate": shared_gate, "shared_up": shared_up, "shared_down": shared_down}


def combine_parts(earlier, later):
    early_real, early_imaginary, early_shift_real, early_shift_imaginary = earlier
    late_real, late_imaginary, late_shift_real, late_shift_imaginary = later
    joint_real = late_real * early_real - late_imaginary * early_imaginary
    joint_imaginary = late_real * early_imaginary + late_imaginary * early_real
    shift_real = late_real * early_shift_real - late_imaginary * early_shift_imaginary + late_shift_real
    shift_imaginary = late_real * early_shift_imaginary + late_imaginary * early_shift_real + late_shift_imaginary
    return (joint_real, joint_imaginary, shift_real, shift_imaginary)

def factors(log_step, states):
    step_rate = jnp.exp(log_step)
    frequency = jnp.pi * jnp.arange(states, dtype=jnp.float32)
    angle = step_rate[:, None] * frequency[None, :]
    turn_cosine = jnp.cos(angle)
    turn_sine = jnp.sin(angle)
    base = jnp.exp(-0.5 * step_rate)[:, None]
    base_real = base * turn_cosine
    starting_quadrature = base * turn_sine
    inverse = 1.0 / (0.25 + frequency * frequency)[None, :]
    lowered = base_real - 1.0
    inject_real = (-0.5 * lowered + starting_quadrature * frequency[None, :]) * inverse
    inject_imaginary = (-0.5 * starting_quadrature - lowered * frequency[None, :]) * inverse
    return (step_rate, turn_cosine, turn_sine, inject_real, inject_imaginary)

def reference(mixer_input, log_step, decay_shift, input_map, readout, mixer_weight, expert_input, norm_gain, routes, route_weight, expert_switch_matrix, up_weight, down_weight, shared_gate, shared_up, shared_down):
    highest = lax.Precision.HIGHEST
    step_rate, turn_cosine, turn_sine, inject_real, inject_imaginary = factors(log_step, STATE)
    blocks_in = mixer_input.reshape(N_EP, MIX_ROWS, GROUPS, GROUP)
    blocks_shift = decay_shift.reshape(N_EP, MIX_ROWS, GROUPS)
    map_real = input_map[0].astype(jnp.float32)
    map_imaginary = input_map[1].astype(jnp.float32)

    def advance(carry, inputs):
        carry_real, carry_imaginary = carry
        block_in, block_shift = inputs
        magnitude = jnp.exp(-0.5 * step_rate[None, :] + block_shift)[:, :, None]
        decay_real = magnitude * turn_cosine[None]
        decay_imaginary = magnitude * turn_sine[None]
        values = block_in.astype(jnp.float32)
        drive_real = jnp.einsum('tgh,gph->tgp', values, map_real, precision=highest)
        drive_imaginary = jnp.einsum('tgh,gph->tgp', values, map_imaginary, precision=highest)
        push_real = inject_real[None] * drive_real - inject_imaginary[None] * drive_imaginary
        push_imaginary = inject_real[None] * drive_imaginary + inject_imaginary[None] * drive_real
        total_real, total_imaginary, local_real, local_imaginary = lax.associative_scan(combine_parts, (decay_real, decay_imaginary, push_real, push_imaginary), axis=0)
        state_real = local_real + total_real * carry_real[None] - total_imaginary * carry_imaginary[None]
        state_imaginary = local_imaginary + total_real * carry_imaginary[None] + total_imaginary * carry_real[None]
        mixed = jnp.einsum('ghp,tgp->tgh', readout[0], state_real, precision=highest) - jnp.einsum('ghp,tgp->tgh', readout[1], state_imaginary, precision=highest)
        return ((state_real[-1], state_imaginary[-1]), mixed.reshape(MIX_ROWS, GROUPS * GROUP))
    start = (jnp.zeros((GROUPS, STATE), jnp.float32), jnp.zeros((GROUPS, STATE), jnp.float32))
    _, outputs = lax.scan(advance, start, (blocks_in, blocks_shift))
    activated = jax.nn.gelu(outputs.reshape(MIX_TOKENS, GROUPS * GROUP)).astype(jnp.bfloat16)
    mixer_out = jnp.dot(activated, mixer_weight, preferred_element_type=jnp.float32).astype(jnp.bfloat16)
    values = expert_input.astype(jnp.float32)
    normed = (values * lax.rsqrt(lax.optimization_barrier(jnp.mean(values * values, axis=-1, keepdims=True)) + 1e-06) * norm_gain).astype(jnp.bfloat16)
    shared_hidden = (jax.nn.silu(jnp.dot(normed, shared_gate, preferred_element_type=jnp.float32)) * jnp.dot(normed, shared_up, preferred_element_type=jnp.float32)).astype(jnp.bfloat16)
    common_contribution = jnp.dot(shared_hidden, shared_down, preferred_element_type=jnp.float32)
    token_count = EXP_TOKENS
    limit = N_EP * CAP
    padded = jnp.concatenate([normed, jnp.zeros((1, D), jnp.bfloat16)], axis=0)

    def expert_step(total, expert):
        chosen = routes == expert
        member = jnp.any(chosen, axis=1)
        weight = lax.optimization_barrier(jnp.sum(jnp.where(chosen, route_weight, 0.0), axis=1))
        position = (jnp.cumsum(member.astype(jnp.int32)) - 1).astype(jnp.int32)
        target = jnp.where(member, position, limit).astype(jnp.int32)
        holder = jnp.full((limit,), token_count, jnp.int32).at[target].set(jnp.arange(token_count, dtype=jnp.int32), mode='drop')
        rows = padded[holder]
        hidden = (jax.nn.silu(jnp.dot(rows, expert_switch_matrix[expert], preferred_element_type=jnp.float32)) * jnp.dot(rows, up_weight[expert], preferred_element_type=jnp.float32)).astype(jnp.bfloat16)
        part = jnp.dot(hidden, down_weight[expert], preferred_element_type=jnp.float32).astype(jnp.bfloat16)
        scale = jnp.concatenate([weight, jnp.zeros((1,), jnp.float32)], axis=0)[holder]
        return (total.at[holder].add(part.astype(jnp.float32) * scale[:, None]), None)
    routed_output, _ = lax.scan(expert_step, jnp.zeros((token_count + 1, D), jnp.float32), jnp.arange(EXPERTS, dtype=jnp.int32))
    experts_out = (common_contribution + routed_output[:token_count]).astype(jnp.bfloat16)
    return (mixer_out, experts_out)
```

```python
import functools

import jax
import jax.numpy as jnp
from jax import lax
from jax.experimental import pallas as pl
from jax.experimental.pallas import tpu as pltpu
from jax.sharding import PartitionSpec as P

F32 = jnp.float32
BF16 = jnp.bfloat16
SEGMENTS = 8
LANES = 128
HIGHEST = lax.Precision.HIGHEST


def call(body, out_shape, flops, moved, megabytes=16, **more):
    return pl.pallas_call(
        body,
        out_shape=out_shape,
        compiler_params=pltpu.CompilerParams(vmem_limit_bytes=megabytes << 20),
        cost_estimate=pl.CostEstimate(flops=flops, bytes_accessed=moved, transcendentals=0),
        **more,
    )


def shape(dims, kind):
    return jax.ShapeDtypeStruct(dims, kind)


def dot(a, b, **more):
    return jnp.dot(a, b, preferred_element_type=F32, **more)


def silu(v):
    return v / (1.0 + jnp.exp(-v))


def slot_places(routes, experts):
    tokens = routes.shape[1]
    expert = lax.broadcasted_iota(jnp.int32, (experts, tokens), 0)
    member = routes[0:1, :] == expert
    for k in range(1, routes.shape[0]):
        member = member | (routes[k : k + 1, :] == expert)
    earlier = lax.broadcasted_iota(jnp.int32, (tokens, tokens), 0)
    later = lax.broadcasted_iota(jnp.int32, (tokens, tokens), 1)
    before = jnp.where(earlier < later, 1.0, 0.0).astype(BF16)
    place = dot(jnp.where(member, 1.0, 0.0).astype(BF16), before)
    return member, place


def dispatch_body(capacity, experts, which_ref, x_ref, gain_ref, routes_ref, normed_ref, out_ref):
    values = x_ref[...].astype(F32)
    mean = jnp.mean(values * values, axis=-1, keepdims=True)
    normed_ref[...] = (values * lax.rsqrt(mean + 1e-06) * gain_ref[...]).astype(BF16)
    member, place = slot_places(routes_ref[...], experts)
    tokens = x_ref.shape[0]
    width = out_ref.shape[1]
    slot = lax.broadcasted_iota(jnp.int32, (capacity, tokens), 0).astype(F32)
    picks = []
    for e in range(experts):
        hit = (slot == place[e : e + 1, :]) & member[e : e + 1, :]
        picks.append(jnp.where(hit, 1.0, 0.0).astype(BF16))
    pick = jnp.concatenate(picks, axis=0)
    start = pl.multiple_of(which_ref[0] * width, width)
    out_ref[...] = dot(pick, normed_ref[:, pl.ds(start, width)]).astype(BF16)


def shared_body(capacity, experts, x_ref, gate_ref, up_ref, routes_ref, weight_ref, hidden_ref, comb_ref):
    x = x_ref[...]
    hidden_ref[...] = (silu(dot(x, gate_ref[...])) * dot(x, up_ref[...])).astype(BF16)
    routes = routes_ref[...]
    weights = weight_ref[...]
    member, place = slot_places(routes, experts)
    tokens = x.shape[0]
    slot = lax.broadcasted_iota(jnp.int32, (capacity, tokens), 0).astype(F32)
    rows = []
    for e in range(experts):
        weight = jnp.where(routes[0:1, :] == e, weights[0:1, :], 0.0)
        for k in range(1, routes.shape[0]):
            weight = weight + jnp.where(routes[k : k + 1, :] == e, weights[k : k + 1, :], 0.0)
        hit = (slot == place[e : e + 1, :]) & member[e : e + 1, :]
        rows.append(jnp.where(hit, weight, 0.0))
    table = jnp.transpose(jnp.concatenate(rows, axis=0))
    for i in range(3):
        piece = table.astype(BF16)
        comb_ref[i] = piece
        table = table - piece.astype(F32)


def combine_body(comb_ref, part_ref, shared_ref, out_ref):
    part = part_ref[...]
    total = dot(comb_ref[0], part) + (dot(comb_ref[1], part) + dot(comb_ref[2], part))
    out_ref[...] = (shared_ref[...] + total).astype(BF16)


def gate_up_first_body(which_ref, rows_ref, gate_ref, up_ref, gate_out, up_out):
    rows = rows_ref[...]
    gate_out[...] = dot(rows, gate_ref[0])
    up_out[...] = dot(rows, up_ref[0])


def gate_up_last_body(which_ref, rows_ref, gate_ref, up_ref, gate_in, up_in, hidden_ref):
    rows = rows_ref[...]
    gate = gate_in[...] + dot(rows, gate_ref[0])
    up = up_in[...] + dot(rows, up_ref[0])
    hidden_ref[...] = (silu(gate) * up).astype(BF16)


def gate_up(which, rows, gate, up, partial, tile=256):
    count, depth = rows.shape
    wide = gate.shape[2]
    tile = min(tile, wide)
    weight_spec = pl.BlockSpec((1, depth, tile), lambda n, w: (0, w[0], n))
    sum_spec = pl.BlockSpec((count, tile), lambda n, w: (0, n))
    specs = [pl.BlockSpec((count, depth), lambda n, w: (0, 0)), weight_spec, weight_spec]
    if partial is None:
        body, ins, kind = gate_up_first_body, (), F32
        outs = [shape((count, wide), F32)] * 2
        out_specs = [sum_spec] * 2
    else:
        body, ins = gate_up_last_body, tuple(partial)
        outs = shape((count, wide), BF16)
        out_specs = sum_spec
        specs = specs + [sum_spec] * 2
    return call(
        body,
        outs,
        4 * count * depth * wide,
        4 * depth * wide,
        megabytes=20,
        grid_spec=pltpu.PrefetchScalarGridSpec(
            num_scalar_prefetch=1, grid=(wide // tile,), in_specs=specs, out_specs=out_specs
        ),
    )(which, rows, gate, up, *ins)


def down_body(last, which_ref, *refs):
    blocks, weight_ref, rest = refs[: len(refs) - 2 - last], refs[len(refs) - 2 - last], refs[-1 - last :]
    out_ref = rest[-1]
    total = rest[0][...] if last else None
    for i, block in enumerate(blocks):
        depth = block.shape[1]
        start = pl.multiple_of(which_ref[i] * depth, depth)
        term = dot(block[...], weight_ref[0, pl.ds(start, depth), :])
        total = term if total is None else total + term
    out_ref[...] = total.astype(out_ref.dtype)


def down(which, blocks, weight, partial, out_kind):
    rows, depth = blocks[0].shape
    wide = weight.shape[2]
    vmem = pl.BlockSpec(memory_space=pltpu.VMEM)
    more = () if partial is None else (partial,)
    return call(
        functools.partial(down_body, len(more)),
        shape((rows, wide), out_kind),
        2 * rows * depth * wide * len(blocks),
        2 * depth * wide * len(blocks),
        megabytes=24,
        in_specs=[pl.BlockSpec(memory_space=pltpu.SMEM)] + [vmem] * (len(blocks) + 1 + len(more)),
        out_specs=vmem,
    )(which, *blocks, weight, *more)


def row_order(rows, by_time):
    steps = rows // SEGMENTS
    a = lax.broadcasted_iota(jnp.int32, (rows, rows), 0)
    b = lax.broadcasted_iota(jnp.int32, (rows, rows), 1)
    placed, time = (b, a) if by_time else (a, b)
    hit = time == (placed % SEGMENTS) * steps + placed // SEGMENTS
    return jnp.where(hit, 1.0, 0.0)


def spread(values, tile, states, width):
    per = LANES // states
    channels = values.shape[0]
    lanes = jnp.concatenate([values] * per, axis=1)
    group = lax.broadcasted_iota(jnp.int32, (channels, LANES), 0) // width
    lane = lax.broadcasted_iota(jnp.int32, (channels, LANES), 1) // states
    return jnp.where(group == tile * per + lane, lanes, jnp.zeros_like(lanes))


def scan_body(states, width, x_ref, shift_ref, const_ref, map_ref, all_ref, local_ref, total_ref, seg_ref):
    rows, channels = x_ref.shape
    merged = const_ref.shape[1]
    steps = rows // SEGMENTS
    per = LANES // states
    order = row_order(rows, False)
    x = dot(order.astype(BF16), x_ref[...]).astype(BF16)
    shift = lax.dot_general(
        order, shift_ref[...], (((1,), (1,)), ((), ())), precision=HIGHEST, preferred_element_type=F32
    )
    lane_group = lax.broadcasted_iota(jnp.int32, (rows, LANES), 1) // states
    for j in range(merged // LANES):
        at = slice(j * LANES, (j + 1) * LANES)
        cosine, sine, inject_re, inject_im, lowered = (const_ref[i : i + 1, at] for i in range(5))
        weight = jnp.concatenate(
            [spread(map_ref[c], j, states, width) for c in range(2)], axis=1
        )
        drive = dot(x, weight)
        drive_re, drive_im = drive[:, :LANES], drive[:, LANES:]
        push_re = inject_re * drive_re - inject_im * drive_im
        push_im = inject_re * drive_im + inject_im * drive_re
        level = jnp.broadcast_to(shift[:, j * per : j * per + 1], (rows, LANES))
        for k in range(1, per):
            column = jnp.broadcast_to(shift[:, j * per + k : j * per + k + 1], (rows, LANES))
            level = jnp.where(lane_group == k, column, level)
        magnitude = jnp.exp(lowered + level)
        decay_re, decay_im = magnitude * cosine, magnitude * sine
        state_re = state_im = total_re = total_im = None
        for s in range(steps):
            r = slice(s * SEGMENTS, (s + 1) * SEGMENTS)
            a, b = decay_re[r], decay_im[r]
            if s == 0:
                state_re, state_im, total_re, total_im = push_re[r], push_im[r], a, b
            else:
                state_re, state_im = (
                    a * state_re - b * state_im + push_re[r],
                    a * state_im + b * state_re + push_im[r],
                )
                total_re, total_im = a * total_re - b * total_im, a * total_im + b * total_re
            local_ref[0, r, at], local_ref[1, r, at] = state_re, state_im
            total_ref[0, r, at], total_ref[1, r, at] = total_re, total_im
        for i, v in enumerate((total_re, total_im, state_re, state_im)):
            seg_ref[i, :, at] = v
        p_re, p_im, s_re, s_im = (v[0:1] for v in (total_re, total_im, state_re, state_im))
        for k in range(1, SEGMENTS):
            a, b, u, v = (w[k : k + 1] for w in (total_re, total_im, state_re, state_im))
            s_re, s_im = a * s_re - b * s_im + u, a * s_im + b * s_re + v
            p_re, p_im = a * p_re - b * p_im, a * p_im + b * p_re
        whole = jnp.concatenate([p_re, p_im, s_re, s_im], axis=0)
        for d in range(all_ref.shape[0]):
            all_ref[d, :, at] = whole


def readout_body(states, width, me_ref, all_ref, local_ref, total_ref, seg_ref, out_w_ref, hidden_ref, out_ref):
    rows, merged = local_ref.shape[1:]
    steps = rows // SEGMENTS
    me = me_ref[0]
    mixed = None
    for j in range(merged // LANES):
        at = slice(j * LANES, (j + 1) * LANES)
        c_re = jnp.zeros((1, LANES), F32)
        c_im = jnp.zeros((1, LANES), F32)
        for d in range(all_ref.shape[0] - 1):
            a, b, u, v = (all_ref[d, i : i + 1, at] for i in range(4))
            n_re, n_im = a * c_re - b * c_im + u, a * c_im + b * c_re + v
            c_re, c_im = jnp.where(d < me, n_re, c_re), jnp.where(d < me, n_im, c_im)
        starts_re, starts_im = [c_re], [c_im]
        for k in range(SEGMENTS - 1):
            a, b, u, v = (seg_ref[i, k : k + 1, at] for i in range(4))
            c_re, c_im = a * c_re - b * c_im + u, a * c_im + b * c_re + v
            starts_re.append(c_re)
            starts_im.append(c_im)
        c_re, c_im = jnp.concatenate(starts_re, axis=0), jnp.concatenate(starts_im, axis=0)
        full_re, full_im = jnp.concatenate([c_re] * steps, axis=0), jnp.concatenate([c_im] * steps, axis=0)
        p_re, p_im = total_ref[0, :, at], total_ref[1, :, at]
        state_re = local_ref[0, :, at] + (p_re * full_re - p_im * full_im)
        state_im = local_ref[1, :, at] + (p_re * full_im + p_im * full_re)
        state = jnp.concatenate([state_re, state_im], axis=1)
        weight = jnp.concatenate(
            [spread(out_w_ref[0], j, states, width), -spread(out_w_ref[1], j, states, width)], axis=1
        )
        high, w_high = state.astype(BF16), weight.astype(BF16)
        low, w_low = (state - high.astype(F32)).astype(BF16), (weight - w_high.astype(F32)).astype(BF16)
        dims = (((1,), (1,)), ((), ()))
        term = functools.partial(lax.dot_general, dimension_numbers=dims, preferred_element_type=F32)
        part = term(high, w_high) + (term(high, w_low) + term(low, w_high))
        mixed = part if mixed is None else mixed + part
    activated = jax.nn.gelu(mixed).astype(BF16)
    activated = dot(row_order(rows, True).astype(BF16), activated).astype(BF16)
    for d in range(out_ref.shape[0]):
        out_ref[d, :rows, :] = activated
        out_ref[d, rows:, :] = hidden_ref[...]


def project_body(rows, all_ref, mixer_ref, shared_ref, mixed_out, shared_out):
    devices, _, width = all_ref.shape
    mixed = common = None
    for d in range(devices):
        at = slice(d * width, (d + 1) * width)
        a = dot(all_ref[d, :rows, :], mixer_ref[at, :])
        b = dot(all_ref[d, rows:, :], shared_ref[at, :])
        mixed, common = (a, b) if d == 0 else (mixed + a, common + b)
    mixed_out[...] = mixed.astype(BF16)
    shared_out[...] = common


def mixer_constants(log_step, states):
    groups = log_step.shape[0]
    merged = groups * states
    step_rate = jnp.exp(jnp.broadcast_to(log_step[:, None], (groups, states)).reshape(1, merged))
    frequency = jnp.pi * (jnp.arange(merged, dtype=jnp.int32) % states).astype(F32)[None, :]
    angle = step_rate * frequency
    cosine, sine = jnp.cos(angle), jnp.sin(angle)
    base = jnp.exp(-0.5 * step_rate)
    base_re, base_im = base * cosine, base * sine
    inverse = 1.0 / (0.25 + frequency * frequency)
    lowered = base_re - 1.0
    inject_re = (-0.5 * lowered + base_im * frequency) * inverse
    inject_im = (-0.5 * base_im - lowered * frequency) * inverse
    return jnp.concatenate([cosine, sine, inject_re, inject_im, -0.5 * step_rate], axis=0)


def shards(
    ep,
    tp,
    mixer_input,
    log_step,
    decay_shift,
    input_map,
    readout,
    mixer_weight,
    expert_input,
    norm_gain,
    routes,
    route_weight,
    expert_switch_matrix,
    up_weight,
    down_weight,
    shared_gate,
    shared_up,
    shared_down,
):
    vmem = pl.BlockSpec(memory_space=pltpu.VMEM)
    smem = pl.BlockSpec(memory_space=pltpu.SMEM)
    my_ep, my_tp = lax.axis_index("ep"), lax.axis_index("tp")
    paired = tp == 4 and ep % 2 == 0
    tokens, features = expert_input.shape
    top = routes.shape[1]
    experts = ep
    capacity = 2 * tokens * top // experts
    slots = experts * capacity
    slice_width = down_weight.shape[2]
    routes_t, weight_t = routes.T, route_weight.T

    halves = 2 if paired else 1
    own = (my_tp ^ (my_tp >> 1)) & 1 if paired else my_tp * 0
    own = own.astype(jnp.int32).reshape(1)
    width = features // halves
    normed, outgoing = call(
        functools.partial(dispatch_body, capacity, experts),
        [shape((tokens, features), BF16), shape((slots, width), BF16)],
        2 * slots * tokens * width,
        4 * tokens * features,
        in_specs=[smem, vmem, vmem, vmem],
        out_specs=[vmem, vmem],
    )(own, expert_input, norm_gain.reshape(1, features), routes_t)
    arrived = lax.all_to_all(
        outgoing.reshape(experts, capacity, width), "ep", split_axis=0, concat_axis=0, tiled=True
    ).reshape(slots, width)

    hidden_width = shared_gate.shape[1]
    shared_hidden, comb = call(
        functools.partial(shared_body, capacity, experts),
        [shape((tokens, hidden_width), BF16), shape((3, tokens, slots), BF16)],
        4 * tokens * features * hidden_width,
        4 * features * hidden_width,
        in_specs=[vmem] * 5,
        out_specs=[vmem] * 2,
    )(normed, shared_gate, shared_up, routes_t, weight_t)

    rows, channels = mixer_input.shape
    groups = log_step.shape[0]
    states, group = input_map.shape[2:]
    merged = groups * states
    map_rows = jnp.transpose(input_map, (0, 1, 3, 2)).reshape(2, channels, states)
    out_rows = readout.reshape(2, channels, states)
    summary, local, total, segment = call(
        functools.partial(scan_body, states, group),
        [
            shape((ep, 4, merged), F32),
            shape((2, rows, merged), F32),
            shape((2, rows, merged), F32),
            shape((4, SEGMENTS, merged), F32),
        ],
        4 * rows * channels * merged,
        16 * rows * merged,
        in_specs=[vmem] * 4,
        out_specs=[vmem] * 4,
    )(mixer_input, decay_shift.T, mixer_constants(log_step, states), map_rows)
    summaries = lax.all_to_all(summary, "ep", split_axis=0, concat_axis=0, tiled=True)
    payload = call(
        functools.partial(readout_body, states, group),
        shape((tp, rows + tokens, channels), BF16),
        12 * rows * channels * merged,
        16 * rows * merged,
        in_specs=[smem] + [vmem] * 6,
        out_specs=vmem,
    )(my_ep.astype(jnp.int32).reshape(1), summaries, local, total, segment, out_rows, shared_hidden)
    spread_payload = lax.all_to_all(payload, "tp", split_axis=0, concat_axis=0, tiled=True)
    mixer_out, common = call(
        functools.partial(project_body, rows),
        [shape((rows, slice_width), BF16), shape((tokens, slice_width), F32)],
        2 * (rows + tokens) * mixer_weight.shape[0] * slice_width,
        4 * mixer_weight.shape[0] * slice_width,
        in_specs=[vmem] * 3,
        out_specs=[vmem] * 2,
    )(spread_payload, mixer_weight, shared_down)

    if paired:
        first = [(e * tp + t, e * tp + (t ^ (1 if e % 2 == 0 else 2))) for e in range(ep) for t in range(tp)]
        second = [(e * tp + t, e * tp + (t ^ (2 if e % 2 == 0 else 1))) for e in range(ep) for t in range(tp)]
        axes = ("ep", "tp")
        other = lax.ppermute(arrived, axes, first)
        partial = gate_up(own, arrived, expert_switch_matrix, up_weight, None)
        hidden = gate_up(1 - own, other, expert_switch_matrix, up_weight, partial)
        near = lax.ppermute(hidden, axes, first)
        side = lax.ppermute(hidden, axes, second)
        far = lax.ppermute(near, axes, second)
        step = jnp.where(my_ep % 2 == 0, 1, 2)
        places = jnp.stack([my_tp, my_tp ^ step, my_tp ^ (3 - step)]).astype(jnp.int32)
        mine = down(places, (hidden, near, side), down_weight, None, F32)
        result = down((my_tp ^ 3).astype(jnp.int32).reshape(1), (far,), down_weight, mine, BF16)
    else:
        gate = dot(arrived, expert_switch_matrix[0])
        up = dot(arrived, up_weight[0])
        hidden = (silu(gate) * up).astype(BF16)
        result = dot(lax.all_gather(hidden, "tp", axis=1, tiled=True), down_weight[0]).astype(BF16)
    returned = lax.all_to_all(
        result.reshape(experts, capacity, slice_width), "ep", split_axis=0, concat_axis=0, tiled=True
    ).reshape(slots, slice_width)
    experts_out = call(
        combine_body,
        shape((tokens, slice_width), BF16),
        6 * tokens * slots * slice_width,
        2 * slots * slice_width,
        in_specs=[vmem] * 3,
        out_specs=vmem,
    )(comb, returned, common)
    return (mixer_out, experts_out)


def solution(mesh):
    placed = (
        P("ep", "tp"),
        P("tp"),
        P("ep", "tp"),
        P(None, "tp", None, None),
        P(None, "tp", None, None),
        P(None, "tp"),
        P("ep", None),
        P(),
        P("ep", None),
        P("ep", None),
        P("ep", None, "tp"),
        P("ep", None, "tp"),
        P("ep", None, "tp"),
        P(None, "tp"),
        P(None, "tp"),
        P(None, "tp"),
    )
    return jax.shard_map(
        functools.partial(shards, mesh.shape["ep"], mesh.shape["tp"]),
        mesh=mesh,
        in_specs=placed,
        out_specs=(P("ep", "tp"), P("ep", "tp")),
        check_vma=False,
    )
```

```python
import functools

import jax
import jax.numpy as jnp
from jax import lax
from jax.experimental import pallas as pl
from jax.experimental.pallas import tpu as pltpu
from jax.sharding import PartitionSpec as P


F32 = jnp.float32
BF16 = jnp.bfloat16
SEGMENTS = 8
LANES = 128
HIGHEST = lax.Precision.HIGHEST


CHUNKS = [[0], [2], [3], [1]]
FULL = [1]


def call(body, out_shape, flops, moved, megabytes=16, **more):
    return pl.pallas_call(
        body,
        out_shape=out_shape,
        compiler_params=pltpu.CompilerParams(vmem_limit_bytes=megabytes << 20),
        cost_estimate=pl.CostEstimate(flops=flops, bytes_accessed=moved, transcendentals=0),
        **more,
    )


def stay(a):
    return pltpu.with_memory_space_constraint(a, pltpu.HBM)


def shape(dims, kind):
    return jax.ShapeDtypeStruct(dims, kind)


def dot(a, b, **more):
    return jnp.dot(a, b, preferred_element_type=F32, **more)


def silu(v):
    return v / (1.0 + jnp.exp(-v))


def slot_places(routes, experts):
    tokens = routes.shape[1]
    expert = lax.broadcasted_iota(jnp.int32, (experts, tokens), 0)
    member = routes[0:1, :] == expert
    for k in range(1, routes.shape[0]):
        member = member | (routes[k : k + 1, :] == expert)
    earlier = lax.broadcasted_iota(jnp.int32, (tokens, tokens), 0)
    later = lax.broadcasted_iota(jnp.int32, (tokens, tokens), 1)
    before = jnp.where(earlier < later, 1.0, 0.0).astype(BF16)
    place = dot(jnp.where(member, 1.0, 0.0).astype(BF16), before)
    return member, place


def expert_at(side, distance, experts):
    me = lax.axis_index("ep")
    core = me % 2 if side == 0 else 1 - me % 2
    return 2 * ((me // 2 + distance) % (experts // 2)) + core


def feature_half(other):
    me = lax.axis_index("tp")
    return (me ^ (me // 2) ^ other) % 2


def picks(named, capacity, member_ref, place_ref, cell):
    tokens = member_ref.shape[1]
    slot = lax.broadcasted_iota(jnp.int32, (capacity, tokens), 0).astype(F32)
    rows = []
    for e in named:
        at = pl.ds(e, 1)
        hit = (slot == place_ref[at, :]) & (member_ref[at, :] > 0.5)
        rows.append(jnp.where(hit, cell(e), 0.0))
    return jnp.concatenate(rows, axis=0)


def note_places(routes_ref, experts, member_ref, place_ref):
    member, place = slot_places(routes_ref[...], experts)
    member_ref[...] = jnp.where(member, 1.0, 0.0)
    place_ref[...] = place


def fetch(sources, targets, sems):
    copies = [pltpu.make_async_copy(a, b, sems.at[i]) for i, (a, b) in enumerate(zip(sources, targets))]
    for copy in copies:
        copy.start()
    return copies


def dispatch_body(capacity, experts, full, routes_hbm, gain_hbm, x_hbm, *rest):
    outs, (member_ref, place_ref, routes_ref, gain_ref, x_ref, sems) = rest[:-6], rest[-6:]
    paired = len(full) > 0
    sources, targets = [routes_hbm, gain_hbm, x_hbm], [routes_ref, gain_ref, x_ref]
    if paired:
        weight_hbm, weight_ref, *outs = outs
        sources, targets = sources + [weight_hbm], targets + [weight_ref]
    normed_ref, *outs = outs
    copies = fetch(sources, targets, sems)
    copies[0].wait()
    note_places(routes_ref, experts, member_ref, place_ref)
    copies[1].wait()
    copies[2].wait()
    values = x_ref[...].astype(F32)
    mean = jnp.mean(values * values, axis=-1, keepdims=True)
    normed_ref[...] = (values * lax.rsqrt(mean + 1e-06) * gain_ref[...]).astype(BF16)
    width = outs[0].shape[1]
    count = experts // len(outs)
    for d, out_ref in enumerate(outs):
        named = [expert_at(d, s, experts) for s in range(count)] if paired else range(experts)
        pick = picks(named, capacity, member_ref, place_ref, lambda e: 1.0).astype(BF16)
        rows = count * capacity
        if not paired:
            out_ref[...] = dot(pick, normed_ref[...]).astype(BF16)
            continue
        start = pl.multiple_of(feature_half(0) * width, width)
        out_ref[:rows, :] = dot(pick, normed_ref[:, pl.ds(start, width)]).astype(BF16)
        start = pl.multiple_of(feature_half(1) * width, width)
        pick = jnp.concatenate([pick[b * capacity : (b + 1) * capacity] for b in full], axis=0)
        out_ref[rows:, :] = dot(pick, normed_ref[:, pl.ds(start, width)]).astype(BF16)
    for copy in copies[3:]:
        copy.wait()


def table_body(capacity, experts, distances, count, *refs):
    sources, rest = refs[:count], refs[count:]
    comb_ref, *carried, routes_ref, weight_ref, member_ref, place_ref, sems = rest
    copies = fetch(sources, [routes_ref, weight_ref, *carried], sems)
    for copy in copies[:2]:
        copy.wait()
    note_places(routes_ref, experts, member_ref, place_ref)
    routes, weights = routes_ref[...], weight_ref[...]

    def cell(e):
        weight = jnp.where(routes[0:1, :] == e, weights[0:1, :], 0.0)
        for k in range(1, routes.shape[0]):
            weight = weight + jnp.where(routes[k : k + 1, :] == e, weights[k : k + 1, :], 0.0)
        return weight

    named = [expert_at(d, s, experts) for s in distances for d in range(2)] if distances else range(experts)
    table = jnp.transpose(picks(named, capacity, member_ref, place_ref, cell))
    for i in range(3):
        piece = table.astype(BF16)
        comb_ref[i] = piece
        table = table - piece.astype(F32)
    for copy in copies[2:]:
        copy.wait()


def shared_body(x_ref, gate_ref, up_ref, hidden_ref):
    x = x_ref[...]
    hidden_ref[...] = (silu(dot(x, gate_ref[...])) * dot(x, up_ref[...])).astype(BF16)


def weigh(comb_ref, parts, first):
    part = jnp.concatenate([p[...] for p in parts], axis=0)
    at = slice(first, first + part.shape[0])
    return dot(comb_ref[0, :, at], part) + (dot(comb_ref[1, :, at], part) + dot(comb_ref[2, :, at], part))


def gather_body(comb_ref, *refs):
    refs[-1][...] = weigh(comb_ref, refs[:-1], 0)


def combine_body(first, sums, comb_ref, *refs):
    total = weigh(comb_ref, refs[sums:-1], first)
    for ref in refs[:sums]:
        total = ref[...] + total
    refs[-1][...] = total.astype(BF16)


def regroup_body(capacity, keep_ref, got_ref, *outs):
    for i, out_ref in enumerate(outs):
        at = slice(i * capacity, (i + 1) * capacity)
        out_ref[:capacity, :] = keep_ref[at, :]
        out_ref[capacity:, :] = got_ref[at, :]


def gate_up_body(count, *refs):
    own, other = refs[:count], refs[count : 2 * count]
    gate_ref, up_ref, hidden_ref = refs[2 * count :]
    depth = own[0].shape[1]
    wide = gate_ref.shape[2]
    tile = min(256, wide)
    first = pl.ds(pl.multiple_of(feature_half(0) * depth, depth), depth)
    second = pl.ds(pl.multiple_of(feature_half(1) * depth, depth), depth)
    a = jnp.concatenate([r[...] for r in own], axis=0)
    b = jnp.concatenate([r[...] for r in other], axis=0)
    for n in range(wide // tile):
        at = slice(n * tile, (n + 1) * tile)
        gate = dot(a, gate_ref[0, first, at]) + dot(b, gate_ref[0, second, at])
        up = dot(a, up_ref[0, first, at]) + dot(b, up_ref[0, second, at])
        hidden_ref[:, at] = (silu(gate) * up).astype(BF16)


def gate_up(own, other, gate, up):
    rows = sum(r.shape[0] for r in own)
    depth, wide = own[0].shape[1], gate.shape[2]
    vmem = pl.BlockSpec(memory_space=pltpu.VMEM)
    return call(
        functools.partial(gate_up_body, len(own)),
        shape((rows, wide), BF16),
        8 * rows * depth * wide,
        8 * depth * wide,
        megabytes=8,
        in_specs=[vmem] * (2 * len(own) + 2),
        out_specs=vmem,
    )(*own, *other, gate, up)


def sources():
    core, me = lax.axis_index("ep") % 2, lax.axis_index("tp")
    return me, me ^ (1 + core), me ^ (2 - core), me ^ 3


def down_body(*refs):
    blocks, weight_ref, outs = refs[:4], refs[4], refs[5:]
    places = sources()
    total = None
    for i, block in enumerate(blocks):
        depth = block.shape[1]
        start = pl.multiple_of(places[i] * depth, depth)
        term = dot(block[...], weight_ref[0, pl.ds(start, depth), :])
        total = term if total is None else total + term
    total = total.astype(BF16)
    rows = outs[0].shape[0]
    for i, out_ref in enumerate(outs):
        out_ref[...] = total[i * rows : (i + 1) * rows]


def down(blocks, weight, pieces):
    rows, depth = blocks[0].shape
    wide = weight.shape[2]
    vmem = pl.BlockSpec(memory_space=pltpu.VMEM)
    return call(
        down_body,
        [shape((rows // pieces, wide), BF16)] * pieces,
        8 * rows * depth * wide,
        8 * depth * wide,
        megabytes=8,
        in_specs=[vmem] * 5,
        out_specs=[vmem] * pieces,
    )(*blocks, weight)


def row_order(rows, by_time):
    steps = rows // SEGMENTS
    a = lax.broadcasted_iota(jnp.int32, (rows, rows), 0)
    b = lax.broadcasted_iota(jnp.int32, (rows, rows), 1)
    placed, time = (b, a) if by_time else (a, b)
    hit = time == (placed % SEGMENTS) * steps + placed // SEGMENTS
    return jnp.where(hit, 1.0, 0.0)


def spread(values, tile, states, width):
    per = LANES // states
    channels = values.shape[0]
    lanes = jnp.concatenate([values] * per, axis=1)
    group = lax.broadcasted_iota(jnp.int32, (channels, LANES), 0) // width
    lane = lax.broadcasted_iota(jnp.int32, (channels, LANES), 1) // states
    return jnp.where(group == tile * per + lane, lanes, jnp.zeros_like(lanes))


def lane_constants(log_step_ref, states, tiles):
    per = LANES // states
    group = lax.broadcasted_iota(jnp.int32, (1, LANES), 1) // states
    rows = []
    for j in range(tiles):
        row = jnp.broadcast_to(log_step_ref[:, j * per : j * per + 1], (1, LANES))
        for k in range(1, per):
            row = jnp.where(group == k, log_step_ref[:, j * per + k : j * per + k + 1], row)
        rows.append(row)
    step_rate = jnp.exp(jnp.concatenate(rows, axis=0))
    frequency = jnp.pi * (lax.broadcasted_iota(jnp.int32, (tiles, LANES), 1) % states).astype(F32)
    angle = step_rate * frequency
    cosine, sine = jnp.cos(angle), jnp.sin(angle)
    base = jnp.exp(-0.5 * step_rate)
    base_re, base_im = base * cosine, base * sine
    inverse = 1.0 / (0.25 + frequency * frequency)
    lowered = base_re - 1.0
    inject_re = (-0.5 * lowered + base_im * frequency) * inverse
    inject_im = (-0.5 * base_im - lowered * frequency) * inverse
    return cosine, sine, inject_re, inject_im, -0.5 * step_rate


def after(earlier, later):
    p, q, u, v = earlier
    a, b, x, y = later
    return a * p - b * q, a * q + b * p, a * u - b * v + x, a * v + b * u + y


def scan_body(states, width, x_ref, shift_ref, log_step_ref, map_ref, all_ref, local_ref, total_ref, seg_ref):
    rows, _ = x_ref.shape
    merged = local_ref.shape[2]
    steps = rows // SEGMENTS
    per = LANES // states
    order = row_order(rows, False)
    x = dot(order.astype(BF16), x_ref[...]).astype(BF16)
    shift = lax.dot_general(
        order, shift_ref[...], (((1,), (1,)), ((), ())), precision=HIGHEST, preferred_element_type=F32
    )
    constants = lane_constants(log_step_ref, states, merged // LANES)
    lane_group = lax.broadcasted_iota(jnp.int32, (rows, LANES), 1) // states
    for j in range(merged // LANES):
        at = slice(j * LANES, (j + 1) * LANES)
        cosine, sine, inject_re, inject_im, lowered = (c[j : j + 1] for c in constants)
        weight = jnp.concatenate([spread(map_ref[c], j, states, width) for c in range(2)], axis=1)
        drive = dot(x, weight)
        drive_re, drive_im = drive[:, :LANES], drive[:, LANES:]
        push_re = inject_re * drive_re - inject_im * drive_im
        push_im = inject_re * drive_im + inject_im * drive_re
        level = jnp.broadcast_to(shift[:, j * per : j * per + 1], (rows, LANES))
        for k in range(1, per):
            column = jnp.broadcast_to(shift[:, j * per + k : j * per + k + 1], (rows, LANES))
            level = jnp.where(lane_group == k, column, level)
        magnitude = jnp.exp(lowered + level)
        decay_re, decay_im = magnitude * cosine, magnitude * sine
        for s in range(steps):
            r = slice(s * SEGMENTS, (s + 1) * SEGMENTS)
            now = decay_re[r], decay_im[r], push_re[r], push_im[r]
            so_far = now if s == 0 else after(so_far, now)
            total_ref[0, r, at], total_ref[1, r, at], local_ref[0, r, at], local_ref[1, r, at] = so_far
        for i, v in enumerate(so_far):
            seg_ref[i, :, at] = v
        whole = tuple(v[0:1] for v in so_far)
        for k in range(1, SEGMENTS):
            whole = after(whole, tuple(v[k : k + 1] for v in so_far))
        whole = jnp.concatenate(whole, axis=0)
        if len(all_ref.shape) == 2:
            all_ref[:, at] = whole
        else:
            for d in range(all_ref.shape[0]):
                all_ref[d, :, at] = whole


def merge_body(mine_ref, partner_ref, out_ref):
    first = lax.axis_index("ep") % 2 == 0
    for j in range(mine_ref.shape[1] // LANES):
        at = slice(j * LANES, (j + 1) * LANES)
        a = tuple(mine_ref[i : i + 1, at] for i in range(4))
        b = tuple(partner_ref[i : i + 1, at] for i in range(4))
        early = tuple(jnp.where(first, x, y) for x, y in zip(a, b))
        late = tuple(jnp.where(first, y, x) for x, y in zip(a, b))
        out_ref[:, at] = jnp.concatenate(after(early, late), axis=0)


def extend_body(before_ref, mine_ref, out_ref):
    first = lax.axis_index("ep") < 2
    for j in range(mine_ref.shape[1] // LANES):
        at = slice(j * LANES, (j + 1) * LANES)
        early = tuple(before_ref[i : i + 1, at] for i in range(4))
        late = tuple(mine_ref[i : i + 1, at] for i in range(4))
        whole = tuple(jnp.where(first, b, w) for w, b in zip(after(early, late), late))
        out_ref[:, at] = jnp.concatenate(whole, axis=0)


def readout_body(states, width, stretches, out_count, *refs):
    links, (local_ref, total_ref, seg_ref, out_w_ref, hidden_ref, out_ref) = refs[:-6], refs[-6:]
    rows, merged = local_ref.shape[1:]
    steps = rows // SEGMENTS
    me = lax.axis_index("ep")
    mixed = None
    for j in range(merged // LANES):
        at = slice(j * LANES, (j + 1) * LANES)
        carried = (jnp.zeros((1, LANES), F32),) * 4
        for read, valid in stretches(links, me):
            new = after(carried, tuple(read(i, at) for i in range(4)))
            carried = tuple(jnp.where(valid, n, c) for n, c in zip(new, carried))
        starts = []
        for k in range(SEGMENTS):
            starts.append(carried)
            if k < SEGMENTS - 1:
                carried = after(carried, tuple(seg_ref[i, k : k + 1, at] for i in range(4)))
        c_re, c_im = (jnp.concatenate([c[i] for c in starts], axis=0) for i in (2, 3))
        full_re, full_im = jnp.concatenate([c_re] * steps, axis=0), jnp.concatenate([c_im] * steps, axis=0)
        p_re, p_im = total_ref[0, :, at], total_ref[1, :, at]
        state_re = local_ref[0, :, at] + (p_re * full_re - p_im * full_im)
        state_im = local_ref[1, :, at] + (p_re * full_im + p_im * full_re)
        state = jnp.concatenate([state_re, state_im], axis=1)
        weight = jnp.concatenate(
            [spread(out_w_ref[0], j, states, width), -spread(out_w_ref[1], j, states, width)], axis=1
        )
        high, w_high = state.astype(BF16), weight.astype(BF16)
        low, w_low = (state - high.astype(F32)).astype(BF16), (weight - w_high.astype(F32)).astype(BF16)
        dims = (((1,), (1,)), ((), ()))
        term = functools.partial(lax.dot_general, dimension_numbers=dims, preferred_element_type=F32)
        part = term(high, w_high) + (term(high, w_low) + term(low, w_high))
        mixed = part if mixed is None else mixed + part
    activated = jax.nn.gelu(mixed).astype(BF16)
    activated = dot(row_order(rows, True).astype(BF16), activated).astype(BF16)
    if out_count is None:
        out_ref[:rows, :] = activated
        out_ref[rows:, :] = hidden_ref[...]
    else:
        for d in range(out_count):
            out_ref[d, :rows, :] = activated
            out_ref[d, rows:, :] = hidden_ref[...]


def project_body(rows, *refs):
    blocks, (mixer_ref, shared_ref, mixed_out, shared_out) = refs[:-4], refs[-4:]
    if len(blocks) > 1:
        reads = list(zip([b[...] for b in blocks], sources()))
    else:
        reads = [(blocks[0][d], d) for d in range(blocks[0].shape[0])]
    mixed = common = None
    for block, place in reads:
        width = block.shape[1]
        at = pl.ds(place * width, width) if isinstance(place, int) else pl.ds(pl.multiple_of(place * width, width), width)
        a = dot(block[:rows], mixer_ref[at, :])
        b = dot(block[rows:], shared_ref[at, :])
        mixed, common = (a, b) if mixed is None else (mixed + a, common + b)
    mixed_out[...] = mixed.astype(BF16)
    shared_out[...] = common


def chip_stretches(links, me):
    valid = me // 2 >= 2, me // 2 >= 1, me % 2 == 1
    return [(lambda i, at, ref=ref: ref[i : i + 1, at], v) for ref, v in zip(links, valid)]


def device_stretches(links, me):
    count = links[0].shape[0]
    return [(lambda i, at, d=d: links[0][d, i : i + 1, at], d < me) for d in range(count - 1)]


def shards(
    ep,
    tp,
    mixer_input,
    log_step,
    decay_shift,
    input_map,
    readout,
    mixer_weight,
    expert_input,
    norm_gain,
    routes,
    route_weight,
    expert_switch_matrix,
    up_weight,
    down_weight,
    shared_gate,
    shared_up,
    shared_down,
):
    vmem = pl.BlockSpec(memory_space=pltpu.VMEM)
    hbm = pl.BlockSpec(memory_space=pltpu.HBM)
    paired = tp == 4 and ep == 8
    tokens, features = expert_input.shape
    top = routes.shape[1]
    experts = ep
    capacity = 2 * tokens * top // experts
    slots = experts * capacity
    slice_width = down_weight.shape[2]
    routes_t, weight_t = routes.T, route_weight.T
    chips = ep // 2

    def swap(a, step, flip):
        pairs = []
        for e in range(ep):
            for t in range(tp):
                there = 2 * ((e // 2 + step) % chips) + (e % 2 ^ flip)
                pairs.append((e * tp + t, there * tp + t))
        return lax.ppermute(a, ("ep", "tp"), pairs)

    def beside(a, even):
        pairs = []
        for e in range(ep):
            for t in range(tp):
                pairs.append((e * tp + t, e * tp + (t ^ (even if e % 2 == 0 else 3 - even))))
        return lax.ppermute(a, ("ep", "tp"), pairs)

    if paired:
        width, full = features // 2, [0] + [b for b in FULL if b < chips]
        out_rows = [(chips + len(full)) * capacity] * 2
    else:
        width, full, out_rows = features, [], [slots]
    carried = [stay(expert_switch_matrix)] if paired else []
    fetched = call(
        functools.partial(dispatch_body, capacity, experts, full),
        [shape(c.shape, BF16) for c in carried]
        + [shape((tokens, features), BF16)]
        + [shape((r, width), BF16) for r in out_rows],
        2 * slots * tokens * width,
        4 * tokens * features,
        megabytes=6,
        in_specs=[hbm] * (3 + len(carried)),
        out_specs=[vmem] * (1 + len(out_rows) + len(carried)),
        scratch_shapes=[pltpu.VMEM((experts, tokens), F32)] * 2
        + [
            pltpu.VMEM((top, tokens), jnp.int32),
            pltpu.VMEM((1, features), F32),
            pltpu.VMEM((tokens, features), BF16),
            pltpu.SemaphoreType.DMA((3 + len(carried),)),
        ],
    )(stay(routes_t), stay(norm_gain.reshape(1, features)), stay(expert_input), *carried)
    if paired:
        gate_here, normed, *outgoing = fetched
    else:
        normed, *outgoing = fetched
    if paired:
        keep, give = outgoing
        got = swap(give, 0, 1)

    rows, channels = mixer_input.shape
    groups = log_step.shape[0]
    states, group = input_map.shape[2:]
    merged = groups * states
    map_rows = jnp.transpose(input_map, (0, 1, 3, 2)).reshape(2, channels, states)
    out_map = readout.reshape(2, channels, states)
    summary, local, total, segment = call(
        functools.partial(scan_body, states, group),
        [
            shape((4, merged) if paired else (ep, 4, merged), F32),
            shape((2, rows, merged), F32),
            shape((2, rows, merged), F32),
            shape((4, SEGMENTS, merged), F32),
        ],
        4 * rows * channels * merged,
        16 * rows * merged,
        megabytes=8,
        in_specs=[vmem] * 4,
        out_specs=[vmem] * 4,
    )(mixer_input, decay_shift.T, log_step.reshape(1, groups), map_rows)
    if paired:
        partner = swap(summary, 0, 1)
        small = dict(megabytes=2, in_specs=[vmem] * 2, out_specs=vmem)
        both = call(merge_body, shape((4, merged), F32), 1, 1, **small)(summary, partner)
        before = swap(both, 1, 0)
        pair = call(extend_body, shape((4, merged), F32), 1, 1, **small)(before, both)
        links = [swap(pair, 2, 0), before, partner]
        stretches = chip_stretches
    else:
        links = [lax.all_to_all(summary, "ep", split_axis=0, concat_axis=0, tiled=True)]
        stretches = device_stretches

    carried = [up_weight] if paired else []
    order = [s for part in CHUNKS for s in part] if paired else []
    comb, *up_here = call(
        functools.partial(table_body, capacity, experts, order, 2 + len(carried)),
        [shape((3, tokens, slots), BF16)] + [shape(c.shape, BF16) for c in carried],
        1,
        1,
        megabytes=4,
        in_specs=[hbm] * (2 + len(carried)),
        out_specs=[vmem] * (1 + len(carried)),
        scratch_shapes=[pltpu.VMEM((top, tokens), jnp.int32), pltpu.VMEM((top, tokens), F32)]
        + [pltpu.VMEM((experts, tokens), F32)] * 2
        + [pltpu.SemaphoreType.DMA((2 + len(carried),))],
    )(*(stay(a) for a in [routes_t, weight_t] + carried))
    hidden_width = shared_gate.shape[1]
    shared_hidden = call(
        shared_body,
        shape((tokens, hidden_width), BF16),
        4 * tokens * features * hidden_width,
        4 * features * hidden_width,
        megabytes=4,
        in_specs=[vmem] * 3,
        out_specs=vmem,
    )(normed, shared_gate, shared_up)

    payload = call(
        functools.partial(readout_body, states, group, stretches, None if paired else tp),
        shape((rows + tokens, channels) if paired else (tp, rows + tokens, channels), BF16),
        12 * rows * channels * merged,
        16 * rows * merged,
        megabytes=8,
        in_specs=[vmem] * (len(links) + 5),
        out_specs=vmem,
    )(*links, local, total, segment, out_map, shared_hidden)
    if paired:
        act_near = beside(payload, 1)
        act_side = beside(payload, 2)
        act_far = beside(act_near, 2)
        acts = [payload, act_near, act_side, act_far]
    else:
        acts = [lax.all_to_all(payload, "tp", split_axis=0, concat_axis=0, tiled=True)]
    mixer_out, common = call(
        functools.partial(project_body, rows),
        [shape((rows, slice_width), BF16), shape((tokens, slice_width), F32)],
        2 * (rows + tokens) * mixer_weight.shape[0] * slice_width,
        4 * mixer_weight.shape[0] * slice_width,
        megabytes=8,
        in_specs=[vmem] * (len(acts) + 2),
        out_specs=[vmem] * 2,
    )(*acts, mixer_weight, shared_down)

    if paired:
        pieces = chips + len(full)
        chunks = call(
            functools.partial(regroup_body, capacity),
            [shape((2 * capacity, width), BF16)] * pieces,
            1,
            4 * keep.size,
            megabytes=4,
            in_specs=[vmem] * 2,
            out_specs=[vmem] * pieces,
        )(keep, got)
        own_rows, other_rows = {0: chunks[0]}, {0: chunks[chips]}
        for s in order[1:]:
            own_rows[s] = swap(chunks[s], s, 0)
            if s in full:
                other_rows[s] = swap(chunks[chips + full.index(s)], s, 0)
            else:
                other_rows[s] = beside(own_rows[s], 1)
        back = {}
        for part in CHUNKS:
            own_part, other_part = [own_rows[s] for s in part], [other_rows[s] for s in part]
            hidden = gate_up(own_part, other_part, gate_here, up_here[0])
            near = beside(hidden, 1)
            side = beside(hidden, 2)
            far = beside(near, 2)
            results = down((hidden, near, side, far), down_weight, 2 * len(part))
            for k, s in enumerate(part):
                back[0, s] = swap(results[2 * k], -s, 0) if s else results[2 * k]
                back[1, s] = swap(results[2 * k + 1], -s, 1)
        parts = [back[d, s] for s in order for d in range(2)]
        late = 2 * len(CHUNKS[-1])
        parts, late = parts[:-late], parts[-late:]
        gathered = call(
            gather_body,
            shape((tokens, slice_width), F32),
            3 * tokens * slots * slice_width,
            slots * slice_width,
            megabytes=4,
            in_specs=[vmem] * (1 + len(parts)),
            out_specs=vmem,
        )(comb, *parts)
        sums, parts, first = [common, gathered], late, slots - len(late) * capacity
    else:
        arrived = lax.all_to_all(
            outgoing[0].reshape(experts, capacity, width), "ep", split_axis=0, concat_axis=0, tiled=True
        ).reshape(slots, width)
        gate = dot(arrived, expert_switch_matrix[0])
        up = dot(arrived, up_weight[0])
        hidden = (silu(gate) * up).astype(BF16)
        result = dot(lax.all_gather(hidden, "tp", axis=1, tiled=True), down_weight[0]).astype(BF16)
        returned = lax.all_to_all(
            result.reshape(experts, capacity, slice_width), "ep", split_axis=0, concat_axis=0, tiled=True
        )
        sums, parts, first = [common], [returned.reshape(slots, slice_width)], 0
    experts_out = call(
        functools.partial(combine_body, first, len(sums)),
        shape((tokens, slice_width), BF16),
        6 * tokens * slots * slice_width,
        2 * slots * slice_width,
        megabytes=8,
        in_specs=[vmem] * (1 + len(sums) + len(parts)),
        out_specs=vmem,
    )(comb, *sums, *parts)
    return (mixer_out, experts_out)


def solution(mesh):
    placed = (
        P("ep", "tp"),
        P("tp"),
        P("ep", "tp"),
        P(None, "tp", None, None),
        P(None, "tp", None, None),
        P(None, "tp"),
        P("ep", None),
        P(),
        P("ep", None),
        P("ep", None),
        P("ep", None, "tp"),
        P("ep", None, "tp"),
        P("ep", None, "tp"),
        P(None, "tp"),
        P(None, "tp"),
        P(None, "tp"),
    )
    return jax.shard_map(
        functools.partial(shards, mesh.shape["ep"], mesh.shape["tp"]),
        mesh=mesh,
        in_specs=placed,
        out_specs=(P("ep", "tp"), P("ep", "tp")),
        check_vma=False,
    )
```
